128 devices in a mesh: fs: 16 (over z, x), tp: 8 (over y, core).
Axes of the slice: x: 4, y: 4, z: 4, core: 2. Of those that a mesh axis runs over, the one named last changes fastest.
Arguments:
- weights: float32 [2, 5632, 2048], P(None, 'fs', 'tp'), may hold values from -6 to 6
- momentum: float32 [2, 5632, 2048], P(None, 'fs', 'tp'), may hold values from -12 to 12
- gradients: float32 [2, 5632, 2048], P(None, 'fs', 'tp'), may hold values from -140 to 140
Outputs:
- new_weights: float32 [2, 5632, 2048], P(None, 'fs', 'tp')
- new_momentum: float32 [2, 5632, 2048], P(None, 'fs', 'tp')
- update: float32 [2, 5632, 2048], P(None, 'fs', 'tp')
The draws below stay inside these ranges and needn't reach their ends.
All inputs are finite; a program needn't handle non-finite values.
Results may differ from the reference program's by a relative error of at most 0.035.
Values may be sent and summed in bfloat16 or wider, within the bound.
No kernel may reach another device: no remote copies, remote signals or barrier semaphores. Data moves between devices by JAX's collectives and lax.ppermute only.
A program may use at most 64 MiB of HBM per device.

```python
import math
import jax
import jax.numpy as jnp
from jax import lax

D = 2048
FF = 5632
MATS = 2
ITERS = 3


def draw_gradients(key, part):
    key_noise, key_rows, key_cols = jax.random.split(key, 3)
    row_ramp = jnp.arange(FF, dtype=jnp.float32) / FF
    col_ramp = jnp.arange(D, dtype=jnp.float32) / D
    row_jitter = jax.random.uniform(key_rows, (MATS, FF, 1), jnp.float32, 0.85, 1.15)
    col_jitter = jax.random.uniform(key_cols, (MATS, 1, D), jnp.float32, 0.9, 1.1)
    row_scale = jnp.power(1.75, row_ramp)[None, :, None] * row_jitter
    col_scale = jnp.power(6.0, col_ramp)[None, None, :] * col_jitter
    noise_draw = jax.random.truncated_normal(key_noise, -4.0, 4.0, (MATS, FF, D), jnp.float32)
    values = 2.5 * noise_draw * row_scale * col_scale
    return values.astype(jnp.float32)


def steps_of(stream_key, extent, cuts, least, high):
    loudness, own = 1.0, jax.random.fold_in(stream_key, 6)
    for axis_at, blocks in cuts:
        draws = jnp.exp(jax.random.uniform(jax.random.fold_in(own, axis_at), (blocks,), jnp.float32, least / len(cuts), high / len(cuts)))
        loudness = loudness * jnp.repeat(draws, extent[axis_at] // blocks).reshape([-1 if axis == axis_at else 1 for axis in range(len(extent))])
    return loudness


def centred(stream_key, shape, width, reach, cuts=(), held_as=jnp.bfloat16):
    factor_of = steps_of(stream_key, shape, cuts, -0.22, 0.18) if cuts else 1.0
    entries = jax.random.normal(stream_key, shape, jnp.float32) * width * factor_of
    return jnp.minimum(jnp.maximum(entries, -reach), reach).astype(held_as)


def setup_inputs(seed: int = 0) -> dict:
    keys = jax.random.split(jax.random.key(seed), 4)
    return {
        "weights": centred(keys[0], (MATS, FF, D), 1.0, 6.0, ((1, 16), (2, 8)), jnp.float32),
        "momentum": centred(keys[1], (MATS, FF, D), 2.0, 12.0, ((1, 16), (2, 8)), jnp.float32),
        "gradients": draw_gradients(jax.random.fold_in(keys[3], 71), 0),
    }


MOMENTUM_DECAY = 0.95
FIRST_COEF = 3.4445
SECOND_COEF = -4.775
THIRD_COEF = 2.0315
LEARN_RATE = 0.02
WEIGHT_DECAY = 0.1
EPSILON = 1e-07
STEP_SCALE = 0.2
NORM_SAFETY = 1.8

def reference(weights, momentum, gradients):
    new_momentum = MOMENTUM_DECAY * momentum + gradients
    iterate = gradients + MOMENTUM_DECAY * new_momentum
    for step in range(ITERS):
        plain = iterate.astype(jnp.bfloat16)
        plain_wide = plain.astype(jnp.float32)
        gram = jnp.einsum('prj,prk->pjk', plain_wide, plain_wide, precision=lax.Precision.HIGHEST)
        gram_bf = gram.astype(jnp.bfloat16)
        gram_wide = gram_bf.astype(jnp.float32)
        if step == 0:
            squares = lax.optimization_barrier(jnp.sum(gram * gram, axis=(1, 2)))
            ratio = (1.0 / (NORM_SAFETY * jnp.sqrt(jnp.sqrt(squares / D)) + EPSILON))[:, None, None]
        else:
            ratio = 1.0
        cubed = jnp.einsum('prk,pkj->prj', plain_wide, gram_wide, precision=lax.Precision.HIGHEST)
        cubed = (cubed * ratio ** 3).astype(jnp.bfloat16)
        folded = jnp.einsum('prk,pkj->prj', cubed.astype(jnp.float32), gram_wide, precision=lax.Precision.HIGHEST)
        iterate = FIRST_COEF * ratio * iterate + SECOND_COEF * cubed.astype(jnp.float32) + THIRD_COEF * (ratio * ratio) * folded
    update = STEP_SCALE * math.sqrt(max(FF, D)) * iterate
    new_weights = weights * (1.0 - LEARN_RATE * WEIGHT_DECAY) - LEARN_RATE * update
    return (new_weights, new_momentum, update)
```

```python
import math

import jax
import jax.numpy as jnp
from jax import lax
from jax.sharding import Mesh, PartitionSpec as P

D = 2048
FF = 5632

MOMENTUM_DECAY = 0.95
A1 = 3.4445
A2 = -4.775
A3 = 2.0315
LEARN_RATE = 0.02
WEIGHT_DECAY = 0.1
EPSILON = 1e-07
STEP_SCALE = 0.2
NORM_SAFETY = 1.8

BF = jnp.bfloat16
F32 = jnp.float32


def gather(value, axes, count):
    spread = jnp.broadcast_to(value[None], (count,) + value.shape)
    return lax.all_to_all(spread, axes, split_axis=0, concat_axis=0, tiled=False)


def swap(value, axis):
    return lax.ppermute(value, axis, [(0, 1), (1, 0)])


def dot(left, right):
    return jnp.dot(left, right, preferred_element_type=F32)


def mul(left, right):
    return dot(left.astype(BF), right)


def mul_split(left, right):
    rows = left.shape[0]
    high = left.astype(BF)
    low = (left - high.astype(F32)).astype(BF)
    both = dot(jnp.concatenate([high, low], 0), right)
    return both[:rows] + both[rows:]


def whole_gram(rows, core):
    part = gather(rows, ("y", "z", "xh"), 32).reshape(D // 2, D)
    other = swap(part, "c")
    first = jnp.where(core == 0, part, other)
    second = jnp.where(core == 0, other, part)
    return jnp.concatenate([first, second], 0)


def per_device(weights, momentum, gradients):
    mat = lax.axis_index("xp")
    core = lax.axis_index("c")
    slot = core * 4 + lax.axis_index("y")

    new_momentum = MOMENTUM_DECAY * momentum + gradients
    iterate = gradients + MOMENTUM_DECAY * new_momentum
    plain = iterate.astype(BF)

    mine = jnp.where(mat == 0, plain[0], plain[1])
    other = jnp.where(mat == 0, plain[1], plain[0])
    block = jnp.concatenate([mine, swap(other, "xp")], 0)

    near = gather(block, "y", 4)
    far = swap(near, "c")
    rows_whole = jnp.concatenate(
        [jnp.where(core == 0, near, far), jnp.where(core == 0, far, near)], 0
    )

    partial = jnp.einsum("ki,nkj->inj", block, rows_whole, preferred_element_type=F32)
    partial = partial.astype(BF).reshape(8, 32, D)
    pieces = lax.all_to_all(partial, ("z", "xh"), split_axis=0, concat_axis=0)
    gram_rows = jnp.sum(pieces.astype(F32), axis=0).astype(BF)

    gram = whole_gram(gram_rows, core)
    squares = jnp.sum(jnp.square(gram.astype(F32)))
    ratio = 1.0 / (NORM_SAFETY * jnp.sqrt(jnp.sqrt(squares / D)) + EPSILON)
    q = ratio * ratio

    g = gram_rows.astype(F32)
    t1 = q * dot(gram_rows, gram)
    hold = q * (A1 * g + A2 * t1 + A3 * q * mul(t1, gram))
    t2 = q * mul(hold, gram)
    next_rows = A1 * hold + q * mul(A2 * hold + A3 * t2, gram)
    gram1 = whole_gram(next_rows.astype(BF), core)

    own = lax.dynamic_slice_in_dim(rows_whole, slot * 88, 88, axis=1)
    own = own.transpose(1, 0, 2).reshape(88, D)
    u = q * dot(own, gram)
    x1 = ratio * (A1 * own.astype(F32) + A2 * u + A3 * q * mul(u, gram))
    x2 = A1 * x1 + mul(A2 * x1 + A3 * mul(x1, gram1), gram1)

    def second_gram(value, product):
        v1 = product(value, gram1)
        v2 = A1 * v1 + product(A2 * v1 + A3 * product(v1, gram1), gram1)
        return A1 * v2 + product(A2 * v2 + A3 * product(v2, gram1), gram1)

    w = second_gram(x2, mul)
    x3 = A1 * x2 + second_gram(A2 * x2 + A3 * w, mul_split)

    back = x3.astype(BF).reshape(88, 8, 256).transpose(1, 0, 2)
    back = lax.all_to_all(back, ("c", "y"), split_axis=0, concat_axis=0).reshape(704, 256)
    kept = back[:352]
    came = swap(back[352:], "xp")
    both = jnp.stack([jnp.where(mat == 0, kept, came), jnp.where(mat == 0, came, kept)])

    update = STEP_SCALE * math.sqrt(max(FF, D)) * both.astype(F32)
    new_weights = weights * (1.0 - LEARN_RATE * WEIGHT_DECAY) - LEARN_RATE * update
    return (new_weights, new_momentum, update)


def solution(mesh):
    fine = Mesh(mesh.devices.reshape(4, 2, 2, 4, 2), ("z", "xh", "xp", "y", "c"))
    spec = P(None, ("z", "xh", "xp"), ("y", "c"))
    return jax.shard_map(
        per_device, mesh=fine, in_specs=(spec, spec, spec), out_specs=(spec, spec, spec), check_vma=False
    )
```

```python
import math

import jax
import jax.numpy as jnp
from jax import lax
from jax.experimental import pallas as pl
from jax.experimental.pallas import tpu as pltpu
from jax.sharding import Mesh, PartitionSpec as P

D = 2048
FF = 5632

MOMENTUM_DECAY = 0.95
A1 = 3.4445
A2 = -4.775
A3 = 2.0315
LEARN_RATE = 0.02
WEIGHT_DECAY = 0.1
EPSILON = 1e-07
STEP_SCALE = 0.2
NORM_SAFETY = 1.8

BF = jnp.bfloat16
F32 = jnp.float32

ROWS = 88
GROWS = 32
BLK = 256
PACK = 5 * BLK
TILE = 512
LOW = 96

VMEM = pl.BlockSpec(memory_space=pltpu.VMEM)
SMEM = pl.BlockSpec(memory_space=pltpu.SMEM)


def at(start, size):
    return pl.ds(pl.multiple_of(start, size), size)


def gather(value, axes, count):
    spread = jnp.broadcast_to(value[None], (count,) + value.shape)
    return lax.all_to_all(spread, axes, split_axis=0, concat_axis=0, tiled=False)


def swap(value, axis):
    return lax.ppermute(value, axis, [(0, 1), (1, 0)])


def unpack(full, own, other, core):
    for part, base in ((own, core * 4), (other, (1 - core) * 4)):

        def panel(k, carry, part=part, base=base):
            here = base + k
            for d in range(5):
                there = lax.rem(here + d, 8)
                block = part[at(k * BLK, BLK), d * BLK : (d + 1) * BLK]
                full[at(here * BLK, BLK), at(there * BLK, BLK)] = block
                if 0 < d < 4:
                    full[at(there * BLK, BLK), at(here * BLK, BLK)] = block.T
            return carry

        lax.fori_loop(0, 4, panel, 0)


def square_sum(parts):
    total = jnp.zeros((1, BLK), F32)
    for part in parts:

        def panel(k, total, part=part):
            for d in range(5):
                block = part[at(k * BLK, BLK), d * BLK : (d + 1) * BLK].astype(F32)
                value = jnp.sum(block * block, axis=0, keepdims=True)
                total = total + (2.0 * value if 0 < d < 4 else value)
            return total

        total = lax.fori_loop(0, 4, panel, total)
    return jnp.sum(total, axis=1, keepdims=True)


def columns(body):
    def step(n, carry):
        body(at(n * TILE, TILE))
        return carry

    lax.fori_loop(0, D // TILE, step, 0)


def dot(left, right):
    return jnp.dot(left, right, preferred_element_type=F32)


def gram_kernel(where, b0, b1, b2, b3, out, rows_out, whole):
    core, half = where[0], where[1]
    slot = core * 2 + half
    away = (1 - core) * 2
    whole[:, at(slot * TILE, TILE)] = b0[...]
    whole[:, at((core * 2 + 1 - half) * TILE, TILE)] = b1[...]
    whole[:, at((away + half) * TILE, TILE)] = b2[...]
    whole[:, at((away + 1 - half) * TILE, TILE)] = b3[...]
    for i in range(2):
        left = b0[:, i * BLK : (i + 1) * BLK].T
        here = slot * 2 + i

        def block(d, carry, i=i, left=left, here=here):
            there = lax.rem(here + d, 8)
            value = dot(left, whole[:, at(there * BLK, BLK)])
            out[i * BLK : (i + 1) * BLK, at(d * BLK, BLK)] = value.astype(BF)
            return carry

        lax.fori_loop(0, 5, block, 0)
    for k in range(4):

        @pl.when(slot == k)
        def _(k=k):
            rows_out[...] = whole[k * ROWS : (k + 1) * ROWS, :]


def first_kernel(where, own, other, plain, rows_out, x_out, full, l1, l2, u, hold, w, g1):
    core, row = where[0], where[1]
    unpack(full, own, other, core)
    squares = square_sum((own, other))
    ratio = 1.0 / (NORM_SAFETY * jnp.sqrt(jnp.sqrt(squares / D)) + EPSILON)
    q = ratio * ratio
    l1[:GROWS, :] = full[at(row, GROWS), :]
    l1[GROWS:, :] = plain[...]

    def one(sl):
        value = q * dot(l1[...], full[:, sl])
        u[:, sl] = value
        l2[:, sl] = value.astype(BF)

    columns(one)

    def two(sl):
        value = q * dot(l2[...], full[:, sl])
        mixed = A1 * l1[:, sl].astype(F32) + A2 * u[:, sl] + A3 * value
        x_out[:, sl] = ratio * mixed[GROWS:]
        kept = q * mixed[:GROWS]
        hold[:, sl] = kept
        l1[:GROWS, sl] = kept.astype(BF)

    columns(two)

    def three(sl):
        value = q * dot(l1[:GROWS, :], full[:, sl])
        w[:, sl] = value
        l2[:GROWS, sl] = value.astype(BF)

    columns(three)

    def four(sl):
        value = q * dot(l2[:GROWS, :], full[:, sl])
        g1[:, sl] = (A1 * hold[:, sl] + A2 * w[:, sl] + A3 * value).astype(BF)

    columns(four)
    here = row // BLK
    for d in range(5):
        rows_out[:, d * BLK : (d + 1) * BLK] = g1[:, at(lax.rem(here + d, 8) * BLK, BLK)]


def second_kernel(where, own, other, x1, out, full, la, lb, v, w, x2, y):
    core = where[0]
    unpack(full, own, other, core)
    lefts = (la, lb)

    def put(left, sl, value, split):
        high = value.astype(BF)
        left[:ROWS, sl] = high
        if split:
            left[LOW : LOW + ROWS, sl] = (value - high.astype(F32)).astype(BF)

    turn = [0]

    def times(finish, split, next_split):
        src, dst = lefts[turn[0]], lefts[1 - turn[0]]
        turn[0] = 1 - turn[0]

        def body(sl):
            if split:
                both = dot(src[...], full[:, sl])
                value = both[:ROWS] + both[LOW : LOW + ROWS]
            else:
                value = dot(src[:ROWS, :], full[:, sl])
            value = finish(sl, value)
            if next_split is not None:
                put(dst, sl, value, next_split)

        columns(body)

    def keep(ref):
        def finish(sl, value):
            ref[:, sl] = value
            return value

        return finish

    def mix(start, ref):
        def finish(sl, value):
            value = A1 * start[:, sl] + A2 * w[:, sl] + A3 * value
            if ref is not None:
                ref[:, sl] = value
            return value

        return finish

    la[ROWS:, :] = jnp.zeros((la.shape[0] - ROWS, D), BF)
    lb[ROWS:, :] = jnp.zeros((lb.shape[0] - ROWS, D), BF)
    la[:ROWS, :] = x1[...].astype(BF)

    times(keep(w), False, False)
    times(mix(x1, x2), False, False)
    s = False
    times(keep(v), s, s)
    times(keep(w), s, s)
    times(mix(v, v), s, s)
    times(keep(w), s, s)
    times(mix(v, y), s, True)
    s = True
    times(keep(v), s, s)
    times(keep(w), s, s)
    times(mix(v, v), s, s)
    times(keep(w), s, s)

    def last(sl, value):
        value = A1 * v[:, sl] + A2 * w[:, sl] + A3 * value
        out[:, sl] = (A1 * x2[:, sl] + A2 * y[:, sl] + A3 * value).astype(BF)
        return None

    times(last, s, None)


def call(kernel, outs, scratch, where, *args):
    return pl.pallas_call(
        kernel,
        out_shape=outs,
        in_specs=[SMEM] + [VMEM] * len(args),
        out_specs=[VMEM] * len(outs),
        scratch_shapes=scratch,
        compiler_params=pltpu.CompilerParams(vmem_limit_bytes=60 * 1024 * 1024),
    )(where, *args)


def shape(dims, dtype):
    return jax.ShapeDtypeStruct(dims, dtype)


def per_device(weights, momentum, gradients):
    mat = lax.axis_index("m")
    core = lax.axis_index("c")
    half = lax.axis_index("y0")
    row = core * 1024 + half * 512 + (lax.axis_index("z") * 4 + lax.axis_index("x")) * GROWS
    where = jnp.stack([core, half]).astype(jnp.int32)
    where_row = jnp.stack([core, row]).astype(jnp.int32)

    new_momentum = MOMENTUM_DECAY * momentum + gradients
    iterate = gradients + MOMENTUM_DECAY * new_momentum
    plain = iterate.astype(BF)

    mine = jnp.where(mat == 0, plain[0], plain[1])
    other = jnp.where(mat == 0, plain[1], plain[0])
    block = jnp.concatenate([mine, swap(other, "m")], 1)
    near = swap(block, "y0")
    far = swap(block, "c")
    diagonal = swap(near, "c")

    partial, own_rows = call(
        gram_kernel,
        (shape((2 * BLK, PACK), BF), shape((ROWS, D), BF)),
        [pltpu.VMEM((352, D), BF)],
        where, block, near, far, diagonal,
    )
    pieces = lax.all_to_all(partial.reshape(16, GROWS, PACK), ("z", "x"), split_axis=0, concat_axis=0)
    gram_rows = jnp.sum(pieces.astype(F32), axis=0).astype(BF)

    def whole(rows):
        part = gather(rows, ("y0", "z", "x"), 32).reshape(1024, PACK)
        return part, swap(part, "c")

    own, away = whole(gram_rows)
    next_rows, x1 = call(
        first_kernel,
        (shape((GROWS, PACK), BF), shape((ROWS, D), F32)),
        [
            pltpu.VMEM((D, D), BF),
            pltpu.VMEM((GROWS + ROWS, D), BF),
            pltpu.VMEM((GROWS + ROWS, D), BF),
            pltpu.VMEM((GROWS + ROWS, D), F32),
            pltpu.VMEM((GROWS, D), F32),
            pltpu.VMEM((GROWS, D), F32),
            pltpu.VMEM((GROWS, D), BF),
        ],
        where_row, own, away, own_rows,
    )
    own, away = whole(next_rows)
    (x3,) = call(
        second_kernel,
        (shape((ROWS, D), BF),),
        [pltpu.VMEM((D, D), BF)]
        + [pltpu.VMEM((2 * LOW, D), BF)] * 2
        + [pltpu.VMEM((ROWS, D), F32)] * 4,
        where_row, own, away, x1,
    )

    back = x3.reshape(ROWS, 4, TILE).transpose(1, 0, 2)
    back = lax.all_to_all(back, ("c", "y0"), split_axis=0, concat_axis=0).reshape(352, TILE)
    kept = back[:, :BLK]
    came = swap(back[:, BLK:], "m")
    both = jnp.stack([jnp.where(mat == 0, kept, came), jnp.where(mat == 0, came, kept)])

    update = STEP_SCALE * math.sqrt(max(FF, D)) * both.astype(F32)
    new_weights = weights * (1.0 - LEARN_RATE * WEIGHT_DECAY) - LEARN_RATE * update
    return (new_weights, new_momentum, update)


def solution(mesh):
    fine = Mesh(mesh.devices.reshape(4, 4, 2, 2, 2), ("z", "x", "m", "y0", "c"))
    spec = P(None, ("z", "x"), ("m", "y0", "c"))
    return jax.shard_map(
        per_device, mesh=fine, in_specs=(spec, spec, spec), out_specs=(spec, spec, spec), check_vma=False
    )
```

```python
import math

import jax
import jax.numpy as jnp
from jax import lax
from jax.experimental import pallas as pl
from jax.experimental.pallas import tpu as pltpu
from jax.sharding import Mesh, PartitionSpec as P

D = 2048
FF = 5632

MOMENTUM_DECAY = 0.95
A1 = 3.4445
A2 = -4.775
A3 = 2.0315
LEARN_RATE = 0.02
WEIGHT_DECAY = 0.1
EPSILON = 1e-07
STEP_SCALE = 0.2
NORM_SAFETY = 1.8

SHIFT = -A2 / (2.0 * A3)
REST = A1 - A3 * SHIFT * SHIFT

BF = jnp.bfloat16
F32 = jnp.float32

ROWS = 88
GROWS = 32
BLK = 128
PANELS = 16
PACK = 9 * BLK
WIDE = 256
TILE = 512

VMEM = pl.BlockSpec(memory_space=pltpu.VMEM)


def at(start, size, align=None):
    return pl.ds(pl.multiple_of(start, align or size), size)


def swap(value, axis):
    return lax.ppermute(value, axis, [(0, 1), (1, 0)])


def unpack(full, own, other, core):
    for part, base in ((own, core * 8), (other, (1 - core) * 8)):

        def panel(k, carry, part=part, base=base):
            here = base + k
            rows = at(k * BLK, BLK)
            for d in range(9):
                there = lax.rem(here + d, PANELS)
                block = part[rows, d * BLK : (d + 1) * BLK]
                full[at(here * BLK, BLK), at(there * BLK, BLK)] = block
                if 0 < d < 8:
                    full[at(there * BLK, BLK), at(here * BLK, BLK)] = block.T
            return carry

        lax.fori_loop(0, 8, panel, 0)


def square_sum(parts):
    total = jnp.zeros((1, BLK), F32)
    for part in parts:

        def panel(k, total, part=part):
            for d in range(9):
                block = part[at(k * BLK, BLK), d * BLK : (d + 1) * BLK].astype(F32)
                value = jnp.sum(block * block, axis=0, keepdims=True)
                total = total + (2.0 * value if 0 < d < 8 else value)
            return total

        total = lax.fori_loop(0, 8, panel, total)
    return jnp.sum(total, axis=1, keepdims=True)


def columns(body):
    def step(n, carry):
        body(n, at(n * TILE, TILE))
        return carry

    lax.fori_loop(0, D // TILE, step, 0)


def dot(left, right):
    return jnp.dot(left, right, preferred_element_type=F32)


def gram_kernel(near, far, out, rows_out, whole):
    core, half = lax.axis_index("c"), lax.axis_index("y0")
    slot = core * 2 + half
    for k in range(4):
        whole[:, at((core * 4 + k) * WIDE, WIDE)] = near[k]
        whole[:, at(((1 - core) * 4 + k) * WIDE, WIDE)] = far[k]
    whole[:, D:] = whole[:, : PACK - BLK]
    for j in range(2):
        left = near[2 * half + j].T
        for i in range(2):
            start = slot * TILE + j * WIDE + i * BLK
            value = dot(left[i * BLK : (i + 1) * BLK], whole[:, at(start, PACK, BLK)])
            out[(2 * j + i) * BLK : (2 * j + i + 1) * BLK, :] = value.astype(BF)
    for k in range(4):

        @pl.when(slot == k)
        def _(k=k):
            rows_out[...] = whole[k * ROWS : (k + 1) * ROWS, :D]


def first_kernel(own, other, plain, rows_out, x_out, full, l1, l2, u, hold, w, g1):
    core = lax.axis_index("c")
    index = lax.axis_index("y0") * 16 + lax.axis_index("z") * 4 + lax.axis_index("x")
    row = core * (D // 2) + index * GROWS
    unpack(full, own, other, core)
    squares = square_sum((own, other))
    ratio = 1.0 / (NORM_SAFETY * jnp.sqrt(jnp.sqrt(squares / D)) + EPSILON)
    q = ratio * ratio
    l1[:GROWS, :] = full[at(row, GROWS), :]
    l1[GROWS:, :] = plain[...]

    def one(n, sl):
        value = q * dot(l1[...], full[:, sl]) - SHIFT * l1[:, sl].astype(F32)
        u[:, sl] = value
        l2[:, sl] = value.astype(BF)

    columns(one)

    def two(n, sl):
        value = q * dot(l2[...], full[:, sl])
        mixed = REST * l1[:, sl].astype(F32) + A3 * (value - SHIFT * u[:, sl])
        x_out[:, sl] = ratio * mixed[GROWS:]
        hold[:, sl] = q * mixed[:GROWS]

    columns(two)
    l1[:GROWS, :] = hold[...].astype(BF)

    def three(n, sl):
        value = q * dot(l1[:GROWS, :], full[:, sl]) - SHIFT * hold[:, sl]
        w[:, sl] = value
        l2[:GROWS, sl] = value.astype(BF)

    columns(three)

    def four(n, sl):
        value = q * dot(l2[:GROWS, :], full[:, sl])
        g1[:, sl] = (REST * hold[:, sl] + A3 * (value - SHIFT * w[:, sl])).astype(BF)

    columns(four)
    here = row // BLK
    packed = jnp.concatenate(
        [g1[:, at(lax.rem(here + d, PANELS) * BLK, BLK)] for d in range(9)], 1
    )

    def spread(i, carry):
        rows_out[i] = packed
        return carry

    lax.fori_loop(0, 32, spread, 0)


def second_kernel(own, other, x1, out, full, la, lb, x2, t, y, z):
    unpack(full, own, other, lax.axis_index("c"))
    lefts = [la, lb]

    def times(finish):
        src, dst = lefts

        def body(n, sl):
            value = finish(sl, dot(src[...], full[:, sl]))
            dst[:, sl] = value.astype(BF)

        columns(body)
        lefts.reverse()

    def keep(sl, value):
        t[:, sl] = value
        return value

    def less(base):
        def finish(sl, value):
            value = value - SHIFT * base[:, sl]
            y[:, sl] = value
            return value

        return finish

    def close(base, ref):
        def finish(sl, value):
            value = REST * base[:, sl] + A3 * (value - SHIFT * y[:, sl])
            ref[:, sl] = value
            return value

        return finish

    def middle(sl, value):
        value = REST * t[:, sl] + A3 * (value - SHIFT * y[:, sl]) - SHIFT * x2[:, sl]
        z[:, sl] = value
        return value

    la[...] = x1[...].astype(BF)
    times(less(x1))
    times(close(x1, x2))
    times(keep)
    times(less(t))
    times(close(t, t))
    times(less(t))
    times(middle)
    times(keep)
    times(less(t))
    times(close(t, t))
    times(less(t))
    src = lefts[0]

    def last(n, sl):
        value = REST * t[:, sl] + A3 * (dot(src[...], full[:, sl]) - SHIFT * y[:, sl])
        value = (REST * x2[:, sl] + A3 * (value - SHIFT * z[:, sl])).astype(BF)
        out[2 * n] = value[:, :WIDE]
        out[2 * n + 1] = value[:, WIDE:]

    columns(last)


def call(kernel, outs, scratch, *args):
    return pl.pallas_call(
        kernel,
        out_shape=outs,
        in_specs=[VMEM] * len(args),
        out_specs=[VMEM] * len(outs),
        scratch_shapes=scratch,
        compiler_params=pltpu.CompilerParams(vmem_limit_bytes=60 * 1024 * 1024),
    )(*args)


def shape(dims, dtype):
    return jax.ShapeDtypeStruct(dims, dtype)


def exchange(value, axes):
    return lax.all_to_all(value, axes, split_axis=0, concat_axis=0)


def per_device(weights, momentum, gradients):
    new_momentum = MOMENTUM_DECAY * momentum + gradients
    iterate = gradients + MOMENTUM_DECAY * new_momentum
    plain = iterate.astype(BF)

    near = exchange(jnp.stack([plain[0], plain[0], plain[1], plain[1]]), ("m", "y0"))
    far = swap(near, "c")
    partial, own_rows = call(
        gram_kernel,
        (shape((TILE, PACK), BF), shape((ROWS, D), BF)),
        [pltpu.VMEM((352, D + PACK - BLK), BF)],
        near, far,
    )
    pieces = exchange(partial.reshape(16, GROWS, PACK), ("z", "x"))
    gram_rows = jnp.sum(pieces.astype(F32), axis=0).astype(BF)

    def whole(spread):
        part = exchange(spread, ("y0", "z", "x")).reshape(D // 2, PACK)
        return part, swap(part, "c")

    own, away = whole(jnp.broadcast_to(gram_rows[None], (32, GROWS, PACK)))
    spread, x1 = call(
        first_kernel,
        (shape((32, GROWS, PACK), BF), shape((ROWS, D), F32)),
        [
            pltpu.VMEM((D, D), BF),
            pltpu.VMEM((GROWS + ROWS, D), BF),
            pltpu.VMEM((GROWS + ROWS, D), BF),
            pltpu.VMEM((GROWS + ROWS, D), F32),
            pltpu.VMEM((GROWS, D), F32),
            pltpu.VMEM((GROWS, D), F32),
            pltpu.VMEM((GROWS, D), BF),
        ],
        own, away, own_rows,
    )
    own, away = whole(spread)
    (x3,) = call(
        second_kernel,
        (shape((8, ROWS, WIDE), BF),),
        [pltpu.VMEM((D, D), BF)]
        + [pltpu.VMEM((ROWS, D), BF)] * 2
        + [pltpu.VMEM((ROWS, D), F32)] * 4,
        own, away, x1,
    )

    back = exchange(x3, ("c", "m", "y0")).reshape(2, 2, 2, ROWS, WIDE)
    both = back.transpose(1, 0, 2, 3, 4).reshape(2, 352, WIDE)

    update = STEP_SCALE * math.sqrt(max(FF, D)) * both.astype(F32)
    new_weights = weights * (1.0 - LEARN_RATE * WEIGHT_DECAY) - LEARN_RATE * update
    return (new_weights, new_momentum, update)


def solution(mesh):
    fine = Mesh(mesh.devices.reshape(4, 4, 2, 2, 2), ("z", "x", "m", "y0", "c"))
    spec = P(None, ("z", "x"), ("m", "y0", "c"))
    return jax.shard_map(
        per_device, mesh=fine, in_specs=(spec, spec, spec), out_specs=(spec, spec, spec), check_vma=False
    )
```

```python
import math

import jax
import jax.numpy as jnp
from jax import lax
from jax.experimental import pallas as pl
from jax.experimental.pallas import tpu as pltpu
from jax.sharding import Mesh, PartitionSpec as P

D = 2048
FF = 5632

MOMENTUM_DECAY = 0.95
A1 = 3.4445
A2 = -4.775
A3 = 2.0315
LEARN_RATE = 0.02
WEIGHT_DECAY = 0.1
EPSILON = 1e-07
STEP_SCALE = 0.2
NORM_SAFETY = 1.8

SHIFT = -A2 / (2.0 * A3)
REST = A1 - A3 * SHIFT * SHIFT

BF = jnp.bfloat16
F32 = jnp.float32

ROWS = 88
GROWS = 32
BLK = 128
PANELS = 16
PACK = 9 * BLK
WIDE = 256
TILE = 512

VMEM = pl.BlockSpec(memory_space=pltpu.VMEM)


def at(start, size, align=None):
    return pl.ds(pl.multiple_of(start, align or size), size)


def swap(value, axis):
    return lax.ppermute(value, axis, [(0, 1), (1, 0)])


def unpack(full, own, other):
    for part, base in ((own, 0), (other, 8)):
        for k in range(8):
            here = base + k
            for d in range(9):
                there = (here + d) % PANELS
                block = part[k * BLK : (k + 1) * BLK, d * BLK : (d + 1) * BLK]
                full[here * BLK : (here + 1) * BLK, there * BLK : (there + 1) * BLK] = block
                if 0 < d < 8:
                    full[there * BLK : (there + 1) * BLK, here * BLK : (here + 1) * BLK] = block.T


def square_sum(parts):
    total = jnp.zeros((1, PACK), F32)
    for part in parts:

        def panel(k, total, part=part):
            block = part[at(k * BLK, BLK), :].astype(F32)
            return total + jnp.sum(block * block, axis=0, keepdims=True)

        total = lax.fori_loop(0, 8, panel, total)
    lane = lax.broadcasted_iota(jnp.int32, (1, PACK), 1)
    twice = jnp.logical_and(lane >= BLK, lane < 8 * BLK)
    return jnp.sum(jnp.where(twice, 2.0 * total, total), axis=1, keepdims=True)


def columns(body):
    for n in range(D // TILE):
        body(n, slice(n * TILE, (n + 1) * TILE))


def dot(left, right):
    return jnp.dot(left, right, preferred_element_type=F32)


def gram_kernel(near, far, out, rows_out, whole):
    core, half = lax.axis_index("c"), lax.axis_index("y0")
    for k in range(4):
        whole[:, k * WIDE : (k + 1) * WIDE] = near[k]
        whole[:, (4 + k) * WIDE : (5 + k) * WIDE] = far[k]
    for j in range(2):
        left = near[2 * half + j].T
        for i in range(2):
            start = half * TILE + j * WIDE + i * BLK
            value = dot(left[i * BLK : (i + 1) * BLK], whole[:, at(start, PACK, BLK)])
            out[(2 * j + i) * BLK : (2 * j + i + 1) * BLK, :] = value.astype(BF)
    for k in range(4):

        @pl.when(core * 2 + half == k)
        def _(k=k):
            rows_out[...] = whole[k * ROWS : (k + 1) * ROWS, :]


def first_kernel(own, other, plain, rows_out, x_out, full, l1, l2, u, hold, w, g1):
    row = (lax.axis_index("y0") * 16 + lax.axis_index("z") * 4 + lax.axis_index("x")) * GROWS
    unpack(full, own, other)
    squares = square_sum((own, other))
    ratio = 1.0 / (NORM_SAFETY * jnp.sqrt(jnp.sqrt(squares / D)) + EPSILON)
    q = ratio * ratio
    l1[:GROWS, :] = full[at(row, GROWS), :]
    l1[GROWS:, :] = plain[...]

    def one(n, sl):
        value = q * dot(l1[...], full[:, sl]) - SHIFT * l1[:, sl].astype(F32)
        u[:, sl] = value
        l2[:, sl] = value.astype(BF)

    columns(one)

    def two(n, sl):
        value = q * dot(l2[...], full[:, sl])
        mixed = REST * l1[:, sl].astype(F32) + A3 * (value - SHIFT * u[:, sl])
        x_out[:, sl] = ratio * mixed[GROWS:]
        hold[:, sl] = q * mixed[:GROWS]

    columns(two)
    l1[:GROWS, :] = hold[...].astype(BF)

    def three(n, sl):
        value = q * dot(l1[:GROWS, :], full[:, sl]) - SHIFT * hold[:, sl]
        w[:, sl] = value
        l2[:GROWS, sl] = value.astype(BF)

    columns(three)

    def four(n, sl):
        value = q * dot(l2[:GROWS, :], full[:, sl])
        g1[:, sl] = (REST * hold[:, sl] + A3 * (value - SHIFT * w[:, sl])).astype(BF)

    columns(four)
    packed = g1[:, at((row // BLK) * BLK, PACK, BLK)]

    def spread(i, carry):
        rows_out[i] = packed
        return carry

    lax.fori_loop(0, 32, spread, 0)


X1, X2, T, Y, Z = range(5)


def second_kernel(own, other, x1, out, full, left, buf):
    core = lax.axis_index("c")
    unpack(full, own, other)
    buf[X1] = x1[...]
    buf[T] = jnp.zeros((ROWS, D), F32)
    buf[Y] = jnp.zeros((ROWS, D), F32)
    left[0] = x1[...].astype(BF)

    def product(i, carry):
        keep = jnp.logical_or(i == 2, i == 7)
        less = (i == 0) | (i == 3) | (i == 5) | (i == 8) | (i == 10)
        scale = jnp.where(jnp.logical_or(keep, less), 1.0, A3)
        scale_base = jnp.where(keep, 0.0, jnp.where(less, -SHIFT, REST))
        scale_y = jnp.where(jnp.logical_or(keep, less), 0.0, -A3 * SHIFT)
        base = jnp.where(i < 2, X1, T)
        into = jnp.where(less, Y, jnp.where(i == 1, X2, jnp.where(i == 6, Z, T)))
        src = lax.rem(i, 2)
        for n in range(D // TILE):
            sl = slice(n * TILE, (n + 1) * TILE)
            value = scale * dot(left[src], full[:, sl])
            value = value + scale_base * buf[base, :, sl] + scale_y * buf[Y, :, sl]
            buf[into, :, sl] = value
            left[1 - src, :, sl] = value.astype(BF)

        @pl.when(i == 6)
        def _():
            value = buf[Z] - SHIFT * buf[X2]
            buf[Z] = value
            left[1 - src] = value.astype(BF)

        return carry

    lax.fori_loop(0, 11, product, 0)
    for n in range(D // TILE):
        sl = slice(n * TILE, (n + 1) * TILE)
        value = dot(left[1], full[:, sl]) - SHIFT * buf[Y, :, sl]
        value = REST * buf[T, :, sl] + A3 * value - SHIFT * buf[Z, :, sl]
        value = (REST * buf[X2, :, sl] + A3 * value).astype(BF)
        for k in range(2):
            out[lax.rem(2 * n + k + core * 4, 8)] = value[:, k * WIDE : (k + 1) * WIDE]


def call(kernel, outs, scratch, limit, *args):
    return pl.pallas_call(
        kernel,
        out_shape=outs,
        in_specs=[VMEM] * len(args),
        out_specs=[VMEM] * len(outs),
        scratch_shapes=scratch,
        compiler_params=pltpu.CompilerParams(vmem_limit_bytes=limit * 1024 * 1024),
    )(*args)


def shape(dims, dtype):
    return jax.ShapeDtypeStruct(dims, dtype)


def exchange(value, axes):
    return lax.all_to_all(value, axes, split_axis=0, concat_axis=0)


def per_device(weights, momentum, gradients):
    new_momentum = MOMENTUM_DECAY * momentum + gradients
    iterate = gradients + MOMENTUM_DECAY * new_momentum
    plain = iterate.astype(BF)

    near = exchange(jnp.stack([plain[0], plain[0], plain[1], plain[1]]), ("m", "y0"))
    far = swap(near, "c")
    partial, own_rows = call(
        gram_kernel,
        (shape((TILE, PACK), BF), shape((ROWS, D), BF)),
        [pltpu.VMEM((352, D), BF)],
        16,
        near, far,
    )
    pieces = exchange(partial.reshape(16, GROWS, PACK), ("z", "x"))
    gram_rows = jnp.sum(pieces.astype(F32), axis=0).astype(BF)

    def whole(spread):
        part = exchange(spread, ("y0", "z", "x")).reshape(D // 2, PACK)
        return part, swap(part, "c")

    own, away = whole(jnp.broadcast_to(gram_rows[None], (32, GROWS, PACK)))
    spread, x1 = call(
        first_kernel,
        (shape((32, GROWS, PACK), BF), shape((ROWS, D), F32)),
        [
            pltpu.VMEM((D, D), BF),
            pltpu.VMEM((GROWS + ROWS, D), BF),
            pltpu.VMEM((GROWS + ROWS, D), BF),
            pltpu.VMEM((GROWS + ROWS, D), F32),
            pltpu.VMEM((GROWS, D), F32),
            pltpu.VMEM((GROWS, D), F32),
            pltpu.VMEM((GROWS, D), BF),
        ],
        32,
        own, away, own_rows,
    )
    own, away = whole(spread)
    (x3,) = call(
        second_kernel,
        (shape((8, ROWS, WIDE), BF),),
        [pltpu.VMEM((D, D), BF), pltpu.VMEM((2, ROWS, D), BF), pltpu.VMEM((5, ROWS, D), F32)],
        32,
        own, away, x1,
    )

    back = exchange(x3, ("c", "m", "y0")).reshape(2, 2, 2, ROWS, WIDE)
    both = back.transpose(1, 0, 2, 3, 4).reshape(2, 352, WIDE)

    update = STEP_SCALE * math.sqrt(max(FF, D)) * both.astype(F32)
    new_weights = weights * (1.0 - LEARN_RATE * WEIGHT_DECAY) - LEARN_RATE * update
    return (new_weights, new_momentum, update)


def solution(mesh):
    fine = Mesh(mesh.devices.reshape(4, 4, 2, 2, 2), ("z", "x", "m", "y0", "c"))
    spec = P(None, ("z", "x"), ("m", "y0", "c"))
    return jax.shard_map(
        per_device, mesh=fine, in_specs=(spec, spec, spec), out_specs=(spec, spec, spec), check_vma=False
    )
```

```python
import math

import jax
import jax.numpy as jnp
from jax import lax
from jax.experimental import pallas as pl
from jax.experimental.pallas import tpu as pltpu
from jax.sharding import Mesh, PartitionSpec as P

D = 2048
FF = 5632

MOMENTUM_DECAY = 0.95
A1 = 3.4445
A2 = -4.775
A3 = 2.0315
LEARN_RATE = 0.02
WEIGHT_DECAY = 0.1
EPSILON = 1e-07
STEP_SCALE = 0.2
NORM_SAFETY = 1.8

SHIFT = -A2 / (2.0 * A3)
REST = A1 - A3 * SHIFT * SHIFT

BF = jnp.bfloat16
F32 = jnp.float32

ROWS = 88
GROWS = 32
BLK = 128
PANELS = 16
PACK = 9 * BLK
WIDE = 256
TILE = 512

VMEM = pl.BlockSpec(memory_space=pltpu.VMEM)


def at(start, size, align=None):
    return pl.ds(pl.multiple_of(start, align or size), size)


def swap(value, axis):
    return lax.ppermute(value, axis, [(0, 1), (1, 0)])


def unpack(full, own, other):
    for part, base in ((own, 0), (other, 8)):
        for k in range(8):
            here = base + k
            for d in range(9):
                there = (here + d) % PANELS
                block = part[k * BLK : (k + 1) * BLK, d * BLK : (d + 1) * BLK]
                full[here * BLK : (here + 1) * BLK, there * BLK : (there + 1) * BLK] = block
                if 0 < d < 8:
                    full[there * BLK : (there + 1) * BLK, here * BLK : (here + 1) * BLK] = block.T


def square_sum(parts):
    total = jnp.zeros((1, PACK), F32)
    for part in parts:

        def panel(k, total, part=part):
            block = part[at(k * BLK, BLK), :].astype(F32)
            return total + jnp.sum(block * block, axis=0, keepdims=True)

        total = lax.fori_loop(0, 8, panel, total)
    lane = lax.broadcasted_iota(jnp.int32, (1, PACK), 1)
    twice = jnp.logical_and(lane >= BLK, lane < 8 * BLK)
    return jnp.sum(jnp.where(twice, 2.0 * total, total), axis=1, keepdims=True)


def columns(body):
    for n in range(D // TILE):
        body(n, slice(n * TILE, (n + 1) * TILE))


def dot(left, right):
    return jnp.dot(left, right, preferred_element_type=F32)


def gram_kernel(near, far, out, rows_out, whole):
    core, half = lax.axis_index("c"), lax.axis_index("y0")
    for k in range(4):
        whole[:, k * WIDE : (k + 1) * WIDE] = near[k]
        whole[:, (4 + k) * WIDE : (5 + k) * WIDE] = far[k]
    for j in range(2):
        left = near[2 * half + j].T
        for i in range(2):
            start = half * TILE + j * WIDE + i * BLK
            value = dot(left[i * BLK : (i + 1) * BLK], whole[:, at(start, PACK, BLK)])
            out[(2 * j + i) * BLK : (2 * j + i + 1) * BLK, :] = value.astype(BF)
    for k in range(4):

        @pl.when(core * 2 + half == k)
        def _(k=k):
            rows_out[...] = whole[k * ROWS : (k + 1) * ROWS, :]


def first_kernel(own, other, plain, rows_out, x_out, full, l1, l2, u, hold, w, g1):
    row = (lax.axis_index("y0") * 16 + lax.axis_index("z") * 4 + lax.axis_index("x")) * GROWS
    unpack(full, own, other)
    squares = square_sum((own, other))
    ratio = 1.0 / (NORM_SAFETY * jnp.sqrt(jnp.sqrt(squares / D)) + EPSILON)
    q = ratio * ratio
    l1[:GROWS, :] = full[at(row, GROWS), :]
    l1[GROWS:, :] = plain[...]

    def one(n, sl):
        value = q * dot(l1[...], full[:, sl]) - SHIFT * l1[:, sl].astype(F32)
        u[:, sl] = value
        l2[:, sl] = value.astype(BF)

    columns(one)

    def two(n, sl):
        value = q * dot(l2[...], full[:, sl])
        mixed = REST * l1[:, sl].astype(F32) + A3 * (value - SHIFT * u[:, sl])
        x_out[:, sl] = ratio * mixed[GROWS:]
        hold[:, sl] = q * mixed[:GROWS]

    columns(two)
    l1[:GROWS, :] = hold[...].astype(BF)

    def three(n, sl):
        value = q * dot(l1[:GROWS, :], full[:, sl]) - SHIFT * hold[:, sl]
        w[:, sl] = value
        l2[:GROWS, sl] = value.astype(BF)

    columns(three)

    def four(n, sl):
        value = q * dot(l2[:GROWS, :], full[:, sl])
        g1[:, sl] = (REST * hold[:, sl] + A3 * (value - SHIFT * w[:, sl])).astype(BF)

    columns(four)
    packed = g1[:, at((row // BLK) * BLK, PACK, BLK)]

    def spread(i, carry):
        rows_out[i] = packed
        return carry

    lax.fori_loop(0, 32, spread, 0)


X2, T, Y, Z = range(4)


def second_kernel(own, other, x1, out, full, left, buf):
    core = lax.axis_index("c")
    unpack(full, own, other)
    left[0] = x1[...].astype(BF)
    turn = [0]

    def times(finish):
        src = turn[0]
        turn[0] = 1 - src

        def body(n, sl):
            value = finish(sl, dot(left[src], full[:, sl]))
            left[1 - src, :, sl] = value.astype(BF)

        columns(body)

    def first_less(sl, value):
        value = value - SHIFT * x1[:, sl]
        buf[Y, :, sl] = value
        return value

    def first_close(sl, value):
        value = REST * x1[:, sl] + A3 * (value - SHIFT * buf[Y, :, sl])
        buf[X2, :, sl] = value
        return value

    def keep(sl, value):
        buf[T, :, sl] = value
        return value

    def less(sl, value):
        value = value - SHIFT * buf[T, :, sl]
        buf[Y, :, sl] = value
        return value

    def close(sl, value):
        value = REST * buf[T, :, sl] + A3 * (value - SHIFT * buf[Y, :, sl])
        buf[T, :, sl] = value
        return value

    def middle(sl, value):
        value = REST * buf[T, :, sl] + A3 * (value - SHIFT * buf[Y, :, sl])
        value = value - SHIFT * buf[X2, :, sl]
        buf[Z, :, sl] = value
        return value

    for finish in (first_less, first_close):
        times(finish)
    for finish in (keep, less, close, less, middle):
        times(finish)
    for finish in (keep, less, close, less):
        times(finish)

    def last(n, sl):
        value = dot(left[turn[0]], full[:, sl]) - SHIFT * buf[Y, :, sl]
        value = REST * buf[T, :, sl] + A3 * value - SHIFT * buf[Z, :, sl]
        value = (REST * buf[X2, :, sl] + A3 * value).astype(BF)
        for k in range(2):
            block = 2 * n + k
            there = lax.rem(block // 4 + core, 2)
            y = block % 4
            out[(y // 2) * 4 + there * 2 + y % 2] = value[:, k * WIDE : (k + 1) * WIDE]

    columns(last)


def call(kernel, outs, scratch, limit, *args):
    return pl.pallas_call(
        kernel,
        out_shape=outs,
        in_specs=[VMEM] * len(args),
        out_specs=[VMEM] * len(outs),
        scratch_shapes=scratch,
        compiler_params=pltpu.CompilerParams(vmem_limit_bytes=limit * 1024 * 1024),
    )(*args)


def shape(dims, dtype):
    return jax.ShapeDtypeStruct(dims, dtype)


def exchange(value, axes):
    return lax.all_to_all(value, axes, split_axis=0, concat_axis=0)


def per_device(weights, momentum, gradients):
    new_momentum = MOMENTUM_DECAY * momentum + gradients
    iterate = gradients + MOMENTUM_DECAY * new_momentum
    plain = iterate.astype(BF)

    near = exchange(jnp.stack([plain[0], plain[0], plain[1], plain[1]]), ("m", "y0"))
    far = swap(near, "c")
    partial, own_rows = call(
        gram_kernel,
        (shape((TILE, PACK), BF), shape((ROWS, D), BF)),
        [pltpu.VMEM((352, D), BF)],
        16,
        near, far,
    )
    pieces = exchange(partial.reshape(16, GROWS, PACK), ("z", "x"))
    gram_rows = jnp.sum(pieces.astype(F32), axis=0).astype(BF)

    def whole(spread):
        part = exchange(spread, ("y0", "z", "x")).reshape(D // 2, PACK)
        return part, swap(part, "c")

    own, away = whole(jnp.broadcast_to(gram_rows[None], (32, GROWS, PACK)))
    spread, x1 = call(
        first_kernel,
        (shape((32, GROWS, PACK), BF), shape((ROWS, D), F32)),
        [
            pltpu.VMEM((D, D), BF),
            pltpu.VMEM((GROWS + ROWS, D), BF),
            pltpu.VMEM((GROWS + ROWS, D), BF),
            pltpu.VMEM((GROWS + ROWS, D), F32),
            pltpu.VMEM((GROWS, D), F32),
            pltpu.VMEM((GROWS, D), F32),
            pltpu.VMEM((GROWS, D), BF),
        ],
        32,
        own, away, own_rows,
    )
    own, away = whole(spread)
    (x3,) = call(
        second_kernel,
        (shape((8, ROWS, WIDE), BF),),
        [pltpu.VMEM((D, D), BF), pltpu.VMEM((2, ROWS, D), BF), pltpu.VMEM((4, ROWS, D), F32)],
        32,
        own, away, x1,
    )

    both = exchange(x3, ("m", "c", "y0")).reshape(2, 352, WIDE)

    update = STEP_SCALE * math.sqrt(max(FF, D)) * both.astype(F32)
    new_weights = weights * (1.0 - LEARN_RATE * WEIGHT_DECAY) - LEARN_RATE * update
    return (new_weights, new_momentum, update)


def solution(mesh):
    fine = Mesh(mesh.devices.reshape(4, 4, 2, 2, 2), ("z", "x", "m", "y0", "c"))
    spec = P(None, ("z", "x"), ("m", "y0", "c"))
    return jax.shard_map(
        per_device, mesh=fine, in_specs=(spec, spec, spec), out_specs=(spec, spec, spec), check_vma=False
    )
```

```python
import math

import jax
import jax.numpy as jnp
from jax import lax
from jax.experimental import pallas as pl
from jax.experimental.pallas import tpu as pltpu
from jax.sharding import Mesh, PartitionSpec as P

D = 2048
FF = 5632

MOMENTUM_DECAY = 0.95
A1 = 3.4445
A2 = -4.775
A3 = 2.0315
LEARN_RATE = 0.02
WEIGHT_DECAY = 0.1
EPSILON = 1e-07
STEP_SCALE = 0.2
NORM_SAFETY = 1.8

SHIFT = -A2 / (2.0 * A3)
REST = A1 - A3 * SHIFT * SHIFT

BF = jnp.bfloat16
F32 = jnp.float32

ROWS = 88
GROWS = 32
BLK = 128
PANELS = 16
PACK = 9 * BLK
WIDE = 256
TILE = 512

VMEM = pl.BlockSpec(memory_space=pltpu.VMEM)


def at(start, size, align=None):
    return pl.ds(pl.multiple_of(start, align or size), size)


def swap(value, axis):
    return lax.ppermute(value, axis, [(0, 1), (1, 0)])


def unpack(full, own, other):
    for part, base in ((own, 0), (other, 8)):
        for k in range(8):
            here = base + k
            for d in range(9):
                there = (here + d) % PANELS
                block = part[k * BLK : (k + 1) * BLK, d * BLK : (d + 1) * BLK]
                full[here * BLK : (here + 1) * BLK, there * BLK : (there + 1) * BLK] = block
                if 0 < d < 8:
                    full[there * BLK : (there + 1) * BLK, here * BLK : (here + 1) * BLK] = block.T


def square_sum(parts):
    total = jnp.zeros((1, PACK), F32)
    for part in parts:

        def panel(k, total, part=part):
            block = part[at(k * BLK, BLK), :].astype(F32)
            return total + jnp.sum(block * block, axis=0, keepdims=True)

        total = lax.fori_loop(0, 8, panel, total)
    lane = lax.broadcasted_iota(jnp.int32, (1, PACK), 1)
    twice = jnp.logical_and(lane >= BLK, lane < 8 * BLK)
    return jnp.sum(jnp.where(twice, 2.0 * total, total), axis=1, keepdims=True)


def columns(body):
    for n in range(D // TILE):
        body(n, slice(n * TILE, (n + 1) * TILE))


def dot(left, right):
    return jnp.dot(left, right, preferred_element_type=F32)


def gram_kernel(near, far, out, rows_out, whole):
    core, half = lax.axis_index("c"), lax.axis_index("y0")
    for k in range(4):
        whole[:, k * WIDE : (k + 1) * WIDE] = near[k]
        whole[:, (4 + k) * WIDE : (5 + k) * WIDE] = far[k]
    for j in range(2):
        left = near[2 * half + j].T
        for i in range(2):
            start = half * TILE + j * WIDE + i * BLK
            value = dot(left[i * BLK : (i + 1) * BLK], whole[:, at(start, PACK, BLK)])
            out[(2 * j + i) * BLK : (2 * j + i + 1) * BLK, :] = value.astype(BF)
    for k in range(4):

        @pl.when(core * 2 + half == k)
        def _(k=k):
            rows_out[...] = whole[k * ROWS : (k + 1) * ROWS, :]


def first_kernel(own, other, q_out, full, scale_out):
    unpack(full, own, other)
    squares = square_sum((own, other))
    ratio = 1.0 / (NORM_SAFETY * jnp.sqrt(jnp.sqrt(squares / D)) + EPSILON)
    scale_out[...] = jnp.broadcast_to(ratio, scale_out.shape)
    q = ratio * ratio

    def panel(k, carry):
        rows = at(k * BLK, BLK)
        value = q * dot(full[rows, :], full[:, at(k * BLK, PACK, BLK)])
        value = q * (A2 * own[rows, :].astype(F32) + A3 * value)
        q_out[rows, :] = value.astype(BF)
        return carry

    lax.fori_loop(0, 8, panel, 0)


def gram_step_kernel(own, other, gram, scale, g1_out, full, h, left):
    unpack(full, own, other)
    ratio = scale[:1, :1]
    q = ratio * ratio

    def panel(k, carry):
        rows = at(k * BLK, BLK)

        def one(n, sl):
            value = dot(gram[rows, :], full[:, sl])
            value = q * (A1 * gram[rows, sl].astype(F32) + value)
            h[:, sl] = value
            left[:, sl] = value.astype(BF)

        columns(one)
        window = at(k * BLK, PACK, BLK)
        value = A1 * h[:, window] + dot(left[...], full[:, window])
        g1_out[rows, :] = value.astype(BF)
        return carry

    lax.fori_loop(0, 8, panel, 0)


def rows_step_kernel(plain, full, scale, out):
    def one(n, sl):
        value = dot(plain[...], full[:, sl])
        out[:, sl] = scale[:1, :1] * (A1 * plain[:, sl].astype(F32) + value)

    columns(one)


X2, T, Y, Z = range(4)


def second_kernel(own, other, x1, out, full, left, buf):
    core = lax.axis_index("c")
    unpack(full, own, other)
    left[0] = x1[...].astype(BF)
    turn = [0]

    def times(finish):
        src = turn[0]
        turn[0] = 1 - src

        def body(n, sl):
            value = finish(sl, dot(left[src], full[:, sl]))
            left[1 - src, :, sl] = value.astype(BF)

        columns(body)

    def first_less(sl, value):
        value = value - SHIFT * x1[:, sl]
        buf[Y, :, sl] = value
        return value

    def first_close(sl, value):
        value = REST * x1[:, sl] + A3 * (value - SHIFT * buf[Y, :, sl])
        buf[X2, :, sl] = value
        return value

    def keep(sl, value):
        buf[T, :, sl] = value
        return value

    def less(sl, value):
        value = value - SHIFT * buf[T, :, sl]
        buf[Y, :, sl] = value
        return value

    def close(sl, value):
        value = REST * buf[T, :, sl] + A3 * (value - SHIFT * buf[Y, :, sl])
        buf[T, :, sl] = value
        return value

    def middle(sl, value):
        value = REST * buf[T, :, sl] + A3 * (value - SHIFT * buf[Y, :, sl])
        value = value - SHIFT * buf[X2, :, sl]
        buf[Z, :, sl] = value
        return value

    for finish in (first_less, first_close):
        times(finish)
    for finish in (keep, less, close, less, middle):
        times(finish)
    for finish in (keep, less, close, less):
        times(finish)

    def last(n, sl):
        value = dot(left[turn[0]], full[:, sl]) - SHIFT * buf[Y, :, sl]
        value = REST * buf[T, :, sl] + A3 * value - SHIFT * buf[Z, :, sl]
        value = (REST * buf[X2, :, sl] + A3 * value).astype(BF)
        for k in range(2):
            block = 2 * n + k
            there = lax.rem(block // 4 + core, 2)
            y = block % 4
            out[(y // 2) * 4 + there * 2 + y % 2] = value[:, k * WIDE : (k + 1) * WIDE]

    columns(last)


def call(kernel, outs, scratch, limit, *args):
    return pl.pallas_call(
        kernel,
        out_shape=outs,
        in_specs=[VMEM] * len(args),
        out_specs=[VMEM] * len(outs),
        scratch_shapes=scratch,
        compiler_params=pltpu.CompilerParams(vmem_limit_bytes=limit * 1024 * 1024),
    )(*args)


def shape(dims, dtype):
    return jax.ShapeDtypeStruct(dims, dtype)


def exchange(value, axes):
    return lax.all_to_all(value, axes, split_axis=0, concat_axis=0)


def per_device(weights, momentum, gradients):
    new_momentum = MOMENTUM_DECAY * momentum + gradients
    iterate = gradients + MOMENTUM_DECAY * new_momentum
    plain = iterate.astype(BF)

    near = exchange(jnp.stack([plain[0], plain[0], plain[1], plain[1]]), ("m", "y0"))
    far = swap(near, "c")
    partial, own_rows = call(
        gram_kernel,
        (shape((TILE, PACK), BF), shape((ROWS, D), BF)),
        [pltpu.VMEM((352, D), BF)],
        16,
        near, far,
    )
    pieces = exchange(partial.reshape(16, GROWS, PACK), ("z", "x"))
    gram_rows = jnp.sum(pieces.astype(F32), axis=0).astype(BF)

    spread = jnp.broadcast_to(gram_rows[None], (32, GROWS, PACK))
    own = exchange(spread, ("y0", "z", "x")).reshape(D // 2, PACK)
    own_q, gram, scale = call(
        first_kernel,
        (shape((D // 2, PACK), BF), shape((D, D), BF), shape((8, BLK), F32)),
        [],
        24,
        own, swap(own, "c"),
    )
    own, factor = call(
        gram_step_kernel,
        (shape((D // 2, PACK), BF), shape((D, D), BF)),
        [pltpu.VMEM((BLK, D), F32), pltpu.VMEM((BLK, D), BF)],
        24,
        own_q, swap(own_q, "c"), gram, scale,
    )
    away = swap(own, "c")
    (x1,) = call(rows_step_kernel, (shape((ROWS, D), F32),), [], 16, own_rows, factor, scale)
    (x3,) = call(
        second_kernel,
        (shape((8, ROWS, WIDE), BF),),
        [pltpu.VMEM((D, D), BF), pltpu.VMEM((2, ROWS, D), BF), pltpu.VMEM((4, ROWS, D), F32)],
        32,
        own, away, x1,
    )

    both = exchange(x3, ("m", "c", "y0")).reshape(2, 352, WIDE)

    update = STEP_SCALE * math.sqrt(max(FF, D)) * both.astype(F32)
    new_weights = weights * (1.0 - LEARN_RATE * WEIGHT_DECAY) - LEARN_RATE * update
    return (new_weights, new_momentum, update)


def solution(mesh):
    fine = Mesh(mesh.devices.reshape(4, 4, 2, 2, 2), ("z", "x", "m", "y0", "c"))
    spec = P(None, ("z", "x"), ("m", "y0", "c"))
    return jax.shard_map(
        per_device, mesh=fine, in_specs=(spec, spec, spec), out_specs=(spec, spec, spec), check_vma=False
    )
```
